32 devices in a mesh: sp: 8 (over z, x), tp: 4 (over y, core).
Axes of the slice: x: 2, y: 2, z: 4, core: 2. Of those that a mesh axis runs over, the one named last changes fastest.
Arguments:
- pool_input: bfloat16 [6144, 1024], P(('sp', 'tp')), may hold values from -6 to 6
- stream_in: bfloat16 [6144, 2048], P(('sp', 'tp')), may hold values from -6 to 6
- group_weight: bfloat16 [4, 256, 256], replicated, may hold values from -0.375 to 0.375
- pool_scale: float32 [1024], replicated, may hold values from 0.1 to 1.9
- out_weight: bfloat16 [1024, 2048], replicated, may hold values from -0.1875 to 0.1875
- norm_gain: float32 [2048], replicated, may hold values from 0.1 to 1.9
- routes: int32 [6144, 2], P(('sp', 'tp')), may hold values from 0 to 31, all different within a row; in each aligned block of 192 rows (0 to 191, 192 to 383, ...) at most 18 rows name the same one
- route_weights: float32 [6144, 2], P(('sp', 'tp')), may hold values from 0.05 to 0.95
- expert_gate: bfloat16 [32, 2048, 1536], P(('sp', 'tp')), may hold values from -0.125 to 0.125
- expert_up: bfloat16 [32, 2048, 1536], P(('sp', 'tp')), may hold values from -0.125 to 0.125
- expert_down: bfloat16 [32, 1536, 2048], P(('sp', 'tp')), may hold values from -0.15625 to 0.15625
Outputs:
- layer_out: bfloat16 [6144, 2048], P(('sp', 'tp'))
The draws below stay inside these ranges and needn't reach their ends.
Inputs may be any that keep to these rules, and one draw needn't show every extreme that they name: `routes`: each row names two different experts. Within each aligned block of 192 rows (the rows of one device) no expert is named more than 18 times, a bound that some block reaches.
All inputs are finite; a program needn't handle non-finite values.
Results may differ from the reference program's by a relative error of at most 0.011.
Values may be sent and summed in bfloat16 or wider, within the bound.
A program may use at most 128 MiB of HBM per device.

```python
import math
import jax
import jax.numpy as jnp
import numpy as np
from jax import lax

D = 2048
POOL = 1024
GROUP = 256
FF = 1536
ROWS = 192
EXPERTS = 32
CAP = 18
TOKENS = 6144


def levels(key, extent, split, low, top_value):
    gain = 1.0
    for dim, shards_of in split:
        steps = jax.random.uniform(jax.random.fold_in(jax.random.fold_in(key, 6), dim), (shards_of,), jnp.float32, low / len(split), top_value / len(split))
        gain = gain * jnp.repeat(jnp.exp(steps), extent[dim] // shards_of).reshape((-1,) + (1,) * (len(extent) - 1 - dim))
    return gain


def assign_block(rng, own, number, rows, count, top, bound, lean):
    ranking = jax.random.permutation(rng, count)
    heavy_load, common = shares(count, rows * top, bound, lean, True), shares(count, rows * top, bound, lean, False)
    places = jnp.arange(count)

    def named(sizes, rotation):
        used = int((sizes > 0).sum())
        fixed = max(1, used // 4)
        shifted = fixed + (places - fixed + rotation * (used - fixed)) % max(1, count - fixed)
        return jnp.zeros((count,), jnp.int32).at[ranking[jnp.where(places < fixed, places, shifted)]].set(jnp.asarray(sizes, jnp.int32))

    sizes = jnp.where(number % 4 == 0, named(heavy_load, number // 4), named(common, number - number // 4 - 1))
    mixed = jax.random.permutation(jax.random.fold_in(own, 3), count)
    source_of, taker = mixed[0:count // 2 * 2:2], mixed[1:count // 2 * 2:2]
    room = jnp.minimum(sizes[source_of] - 1, bound - sizes[taker]) // 2
    room = jnp.where((source_of == ranking[0]) | (taker == ranking[0]) | (sizes[taker] == 0), 0, jnp.maximum(room, 0))
    shifted = jax.random.randint(jax.random.fold_in(own, 4), (count // 2,), 0, 1 << 20) % (room + 1)
    sizes = sizes.at[source_of].add(-shifted).at[taker].add(shifted)
    items = jnp.searchsorted(jnp.cumsum(sizes), jnp.arange(rows * top), side="right").astype(jnp.int32)
    table = items.reshape(top, rows).T
    table = table[jax.random.permutation(jax.random.fold_in(own, 1), rows)]
    rotation = jax.random.randint(jax.random.fold_in(own, 2), (rows, 1), 0, top)
    return jnp.take_along_axis(table, (jnp.arange(top)[None, :] + rotation) % top, axis=1)


def shares(count, total, most, lean, full):
    weights = [(1 << 20) // math.isqrt(rank ** lean) + 1 for rank in range(1, count + 1)]
    largest = most if full else min(most, max(-(-total // count), total * weights[0] // sum(weights)))
    least = 1 if total - largest >= count - 1 else 0
    counts, surplus = [largest] + [least] * (count - 1), total - largest - least * (count - 1)
    while surplus > 0:
        movable = [i for i in range(1, count) if counts[i] < largest] or [i for i in range(1, count) if counts[i] < most]
        pool, budget = sum([weights[i] for i in movable]), surplus
        for i in movable:
            more = min(most - counts[i], max(1, budget * weights[i] // pool), surplus)
            counts[i] = counts[i] + more
            surplus = surplus - more
    return np.array(counts)


def normal_values(own_key, shape, spread, bound, shards=(), held_as=jnp.bfloat16):
    entries = jax.random.normal(own_key, shape, jnp.float32) * spread
    if len(shards) > 0:
        entries = levels(own_key, shape, shards, -0.22, 0.18) * entries
    return jnp.clip(entries, min=-bound, max=bound).astype(held_as)


def setup_inputs(seed: int = 0) -> dict:
    key_list = jax.random.split(jax.random.key(seed), 12)
    pool_input = normal_values(key_list[0], (TOKENS, POOL), 1.0, 6.0, ((0, 32),))
    stream_in = normal_values(key_list[1], (TOKENS, D), 1.0, 6.0, ((0, 32),))
    group_weight = normal_values(key_list[2], (4, GROUP, GROUP), GROUP ** -0.5, 0.375)
    pool_scale = jnp.clip(1.0 + 0.18 * jax.random.normal(key_list[3], (POOL,), jnp.float32), 0.1, 1.9)
    out_weight = normal_values(key_list[4], (POOL, D), POOL ** -0.5, 0.1875)
    norm_gain = jnp.clip(1.0 + 0.18 * jax.random.normal(key_list[5], (D,), jnp.float32), 0.1, 1.9)
    routes_keys = jax.random.split(jax.random.fold_in(key_list[6], 1), TOKENS // ROWS)
    routes_turns = jax.random.permutation(jax.random.fold_in(key_list[6], 3), TOKENS // ROWS)
    routes = jax.vmap(lambda own, number: assign_block(jax.random.fold_in(key_list[6], 2), own, number, ROWS, EXPERTS, 2, CAP, 0))(routes_keys, routes_turns).reshape((TOKENS, 2))
    route_weights = jnp.clip(0.05 + 0.9 * jax.random.uniform(key_list[7], (TOKENS, 2), jnp.float32) ** levels(key_list[7], (TOKENS, 2), ((0, 32),), -0.2, 0.2), 0.05, 0.95)
    expert_gate = normal_values(key_list[8], (EXPERTS, D, FF), D ** -0.5, 0.125, ((0, 32),))
    expert_up = normal_values(key_list[9], (EXPERTS, D, FF), D ** -0.5, 0.125, ((0, 32),))
    expert_down = normal_values(key_list[10], (EXPERTS, FF, D), FF ** -0.5, 0.15625, ((0, 32),))
    return dict(pool_input=pool_input, stream_in=stream_in, group_weight=group_weight, pool_scale=pool_scale, out_weight=out_weight, norm_gain=norm_gain, routes=routes, route_weights=route_weights, expert_gate=expert_gate, expert_up=expert_up, expert_down=expert_down)


pool_windows = (2, 4, 8, 16)
reach_rows = 15
norm_epsilon = 1e-05

def pooling_mixer(pool_input, group_weight, pool_scale):
    total_rows = pool_input.shape[0]
    group_width = pool_input.shape[1] // 4
    values = pool_input.astype(jnp.float32)
    padded = jnp.pad(values, ((reach_rows, 0), (0, 0)))
    position = jnp.arange(total_rows, dtype=jnp.float32)[:, None]
    pieces = []
    for group_index, window in enumerate(pool_windows):
        low = group_index * group_width
        high = low + group_width
        trail = jnp.zeros((total_rows, group_width), jnp.float32)
        for lag_step in range(window):
            trail = trail + padded[reach_rows - lag_step:reach_rows - lag_step + total_rows, low:high]
        count = jnp.minimum(position + 1.0, float(window))
        pooled = (trail / count - values[:, low:high]).astype(jnp.bfloat16)
        mapped = jnp.dot(pooled, group_weight[group_index], preferred_element_type=jnp.float32)
        pieces.append((mapped * pool_scale[low:high]).astype(jnp.bfloat16))
    return jnp.concatenate(pieces, axis=1)

def reference(pool_input, stream_in, group_weight, pool_scale, out_weight, norm_gain, routes, route_weights, expert_gate, expert_up, expert_down):
    total_rows = pool_input.shape[0]
    width = stream_in.shape[1]
    grouped = pooling_mixer(pool_input, group_weight, pool_scale)
    stream = (stream_in.astype(jnp.float32) + jnp.dot(grouped, out_weight, preferred_element_type=jnp.float32)).astype(jnp.bfloat16)
    stream_f = stream.astype(jnp.float32)
    scale = lax.rsqrt(lax.optimization_barrier(jnp.mean(stream_f * stream_f, axis=1, keepdims=True)) + norm_epsilon)
    normed = (stream_f * scale * norm_gain).astype(jnp.bfloat16)
    block_count = total_rows // ROWS

    def block_slots(block_routes):
        assigned = block_routes.reshape(-1)
        one_hot = (assigned[:, None] == jnp.arange(EXPERTS, dtype=jnp.int32)[None, :]).astype(jnp.int32)
        earlier = lax.optimization_barrier(jnp.sum((jnp.cumsum(one_hot, axis=0) - one_hot) * one_hot, axis=1))
        return (assigned * CAP + earlier).astype(jnp.int32)
    slot_index = jax.vmap(block_slots)(routes.reshape(block_count, ROWS, 2))
    owner = (jnp.arange(2 * ROWS, dtype=jnp.int32) // 2).astype(jnp.int32)

    def block_table(slots):
        return jnp.full((EXPERTS * CAP,), ROWS, jnp.int32).at[slots].set(owner)
    slot_rows = jax.vmap(block_table)(slot_index)
    normed_blocks = jnp.concatenate([normed.reshape(block_count, ROWS, width), jnp.zeros((block_count, 1, width), jnp.bfloat16)], axis=1)

    def serve(expert_id):
        picks = lax.dynamic_slice_in_dim(slot_rows, (expert_id * CAP).astype(jnp.int32), CAP, axis=1)
        inputs = jnp.take_along_axis(normed_blocks, picks[:, :, None], axis=1).reshape(-1, width)
        gate = jnp.dot(inputs, expert_gate[expert_id], preferred_element_type=jnp.float32)
        upward = jnp.dot(inputs, expert_up[expert_id], preferred_element_type=jnp.float32)
        hidden = (jax.nn.silu(gate) * upward).astype(jnp.bfloat16)
        result = jnp.dot(hidden, expert_down[expert_id], preferred_element_type=jnp.float32).astype(jnp.bfloat16)
        return result.reshape(block_count, CAP, width)
    answers = lax.map(serve, jnp.arange(EXPERTS, dtype=jnp.int32))
    answers = answers.transpose(1, 0, 2, 3).reshape(block_count, EXPERTS * CAP, width)
    picked = jnp.take_along_axis(answers, slot_index[:, :, None], axis=1).reshape(total_rows, 2, width)
    combined = stream_f + route_weights[:, 0:1] * picked[:, 0].astype(jnp.float32) + route_weights[:, 1:2] * picked[:, 1].astype(jnp.float32)
    return combined.astype(jnp.bfloat16)
```

```python
import functools

import jax
import jax.numpy as jnp
from jax import lax
from jax.experimental import pallas as pl
from jax.experimental.pallas import tpu as pltpu
from jax.sharding import PartitionSpec as P

MESH = pl.DeviceIdType.MESH
pool_windows = (2, 4, 8, 16)
halo_rows = 16
norm_epsilon = 1e-05
groups = 4
visit_order = (0, 2, 1, 3)
chunk = 256


def kernel(
    n,
    tp_size,
    main,
    extra,
    pool_hbm,
    stream_hbm,
    group_hbm,
    scale_ref,
    out_hbm,
    gain_ref,
    slot_rows_ref,
    slot_cols_ref,
    route_weights_ref,
    gate_hbm,
    up_hbm,
    down_hbm,
    result_ref,
    pool_buf,
    halo_buf,
    extended,
    stream_buf,
    group_buf,
    outw_buf,
    gate_buf,
    up_buf,
    down_buf,
    normed_buf,
    grouped_buf,
    total,
    hidden_buf,
    sent,
    arrived,
    answer,
    returned,
    sent_x,
    arrived_x,
    answer_x,
    returned_x,
    load_sem,
    halo_send,
    halo_recv,
    own_sem,
    send_sem,
    recv_sem,
):
    f32, bf16 = jnp.float32, jnp.bfloat16
    rows, width = result_ref.shape
    pool_width = pool_buf.shape[1]
    group_width = pool_width // 4
    ff = hidden_buf.shape[1]
    size = n // groups
    per_group = size * (main + extra)
    edge = size * main

    me = lax.axis_index("sp") * tp_size + lax.axis_index("tp")
    my_group = me // size
    my_place = me % size

    def coordinates(device):
        return (device // tp_size, device % tp_size)

    loads = []
    for number, (source, target) in enumerate(
        (
            (pool_hbm, pool_buf),
            (group_hbm, group_buf),
            (out_hbm, outw_buf),
            (stream_hbm, stream_buf),
            (gate_hbm.at[0], gate_buf),
            (up_hbm.at[0], up_buf),
            (down_hbm.at[0], down_buf),
        )
    ):
        copy = pltpu.make_async_copy(source, target, load_sem.at[number])
        copy.start()
        loads.append(copy)

    barrier = pltpu.get_barrier_semaphore()

    def greet(step, carry):
        pl.semaphore_signal(
            barrier, inc=1, device_id=coordinates((me + step) % n), device_id_type=MESH
        )
        return carry

    lax.fori_loop(1, n, greet, 0)
    pl.semaphore_wait(barrier, n - 1)

    halo = pltpu.make_async_remote_copy(
        src_ref=pool_hbm.at[pl.ds(rows - halo_rows, halo_rows)],
        dst_ref=halo_buf,
        send_sem=halo_send,
        recv_sem=halo_recv,
        device_id=coordinates((me + 1) % n),
        device_id_type=MESH,
    )
    halo.start()

    loads[0].wait()
    extended[pl.ds(halo_rows, rows), :] = pool_buf[...].astype(f32)
    loads[1].wait()
    halo.wait()
    extended[pl.ds(0, halo_rows), :] = jnp.where(me > 0, halo_buf[...].astype(f32), 0.0)
    position = (me * rows + lax.broadcasted_iota(jnp.int32, (rows, 1), 0)).astype(f32)
    for index, window in enumerate(pool_windows):
        low = index * group_width
        columns = slice(low, low + group_width)
        own = extended[pl.ds(halo_rows, rows), columns]
        trail = own
        for lag in range(1, window):
            trail = trail + extended[pl.ds(halo_rows - lag, rows), columns]
        count = jnp.minimum(position + 1.0, float(window))
        pooled = (trail / count - own).astype(bf16)
        mapped = jnp.dot(pooled, group_buf[index], preferred_element_type=f32)
        grouped_buf[:, columns] = (mapped * scale_ref[:, columns]).astype(bf16)

    loads[2].wait()
    loads[3].wait()

    def project(step, square):
        columns = pl.ds(pl.multiple_of(step * chunk, chunk), chunk)
        value = stream_buf[:, columns].astype(f32) + jnp.dot(
            grouped_buf[...], outw_buf[:, columns], preferred_element_type=f32
        )
        value = value.astype(bf16).astype(f32)
        total[:, columns] = value
        return square + jnp.sum(value * value, axis=1, keepdims=True)

    square = lax.fori_loop(0, width // chunk, project, jnp.zeros((rows, 1), f32))
    scale = lax.rsqrt(square / width + norm_epsilon)
    normed_buf[...] = (total[...] * scale * gain_ref[...]).astype(bf16)

    def block(buffer, group, place):
        return buffer.at[group, pl.ds(pl.multiple_of(place * main, 16), main)]

    def spread(buffer, buffer_x, group):
        if not extra:
            return
        for place in range(size):
            start = edge + place * extra
            buffer_x[group * size + place] = buffer[group, start : start + extra, :]

    def gather(buffer, buffer_x, group):
        if not extra:
            return
        for place in range(size):
            start = edge + place * extra
            buffer[group, start : start + extra, :] = buffer_x[group * size + place]

    def exchange(way, source, source_x, target, target_x, group, first):
        def one(step, carry):
            place = (my_place + step) % size
            peer = group * size + place
            if main:
                pltpu.make_async_remote_copy(
                    src_ref=block(source, group, place),
                    dst_ref=block(target, my_group, my_place),
                    send_sem=send_sem.at[way, 0, group],
                    recv_sem=recv_sem.at[way, 0, my_group],
                    device_id=coordinates(peer),
                    device_id_type=MESH,
                ).start()
            if extra:
                pltpu.make_async_remote_copy(
                    src_ref=source_x.at[peer],
                    dst_ref=target_x.at[me],
                    send_sem=send_sem.at[way, 1, group],
                    recv_sem=recv_sem.at[way, 1, my_group],
                    device_id=coordinates(peer),
                    device_id_type=MESH,
                ).start()
            return carry

        lax.fori_loop(first, size, one, 0)

    def own_block(way, source, source_x, target, target_x):
        copies = []
        if main:
            copies.append(
                pltpu.make_async_copy(
                    block(source, my_group, my_place),
                    block(target, my_group, my_place),
                    own_sem.at[way, 0],
                )
            )
        if extra:
            copies.append(
                pltpu.make_async_copy(source_x.at[me], target_x.at[me], own_sem.at[way, 1])
            )
        return copies

    def finish(semaphore, way, buffer, buffer_x, group, count):
        if main:
            span = buffer.at[group, pl.ds(0, count * main)]
            pltpu.make_async_copy(span, span, semaphore.at[way, 0, group]).wait()
        if extra:
            span = buffer_x.at[pl.ds(group * size, count)]
            pltpu.make_async_copy(span, span, semaphore.at[way, 1, group]).wait()

    own_out = own_block(0, sent, sent_x, arrived, arrived_x)
    own_back = own_block(1, answer, answer_x, returned, returned_x)

    for turn in visit_order:
        group = (my_group + turn) % groups
        wanted = group * per_group + lax.broadcasted_iota(jnp.int32, (per_group, rows), 0)
        chosen = (wanted == slot_rows_ref[0:1, :]) | (wanted == slot_rows_ref[1:2, :])
        chosen = jnp.where(chosen, 1.0, 0.0).astype(bf16)

        def pick(step, carry, group=group, chosen=chosen):
            columns = pl.ds(pl.multiple_of(step * chunk, chunk), chunk)
            sent[group, :, columns] = jnp.dot(
                chosen, normed_buf[:, columns], preferred_element_type=f32
            ).astype(bf16)
            return carry

        lax.fori_loop(0, width // chunk, pick, 0)
        spread(sent, sent_x, group)
        exchange(0, sent, sent_x, arrived, arrived_x, group, 1 if turn == 0 else 0)
        if turn == 0:
            for copy in own_out:
                copy.start()

    for copy in loads[4:]:
        copy.wait()

    for turn in visit_order:
        group = (my_group + groups - turn) % groups
        finish(recv_sem, 0, arrived, arrived_x, group, size - 1 if turn == 0 else size)
        if turn == 0:
            for copy in own_out:
                copy.wait()
        gather(arrived, arrived_x, group)

        def hide(step, carry, group=group):
            columns = pl.ds(pl.multiple_of(step * chunk, chunk), chunk)
            inputs = arrived[group]
            gate = jnp.dot(inputs, gate_buf[:, columns], preferred_element_type=f32)
            upward = jnp.dot(inputs, up_buf[:, columns], preferred_element_type=f32)
            hidden_buf[:, columns] = (gate / (1.0 + jnp.exp(-gate)) * upward).astype(bf16)
            return carry

        lax.fori_loop(0, ff // chunk, hide, 0)

        def lower(step, carry, group=group):
            columns = pl.ds(pl.multiple_of(step * chunk, chunk), chunk)
            answer[group, :, columns] = jnp.dot(
                hidden_buf[...], down_buf[:, columns], preferred_element_type=f32
            ).astype(bf16)
            return carry

        lax.fori_loop(0, width // chunk, lower, 0)
        spread(answer, answer_x, group)
        exchange(1, answer, answer_x, returned, returned_x, group, 1 if turn == 0 else 0)
        if turn == 0:
            for copy in own_back:
                copy.start()

    for turn in visit_order:
        group = (my_group + turn) % groups
        finish(recv_sem, 1, returned, returned_x, group, size - 1 if turn == 0 else size)
        if turn == 0:
            for copy in own_back:
                copy.wait()
        gather(returned, returned_x, group)
        offered = group * per_group + lax.broadcasted_iota(jnp.int32, (rows, per_group), 1)
        mix = jnp.where(offered == slot_cols_ref[:, 0:1], route_weights_ref[:, 0:1], 0.0)
        mix = mix + jnp.where(offered == slot_cols_ref[:, 1:2], route_weights_ref[:, 1:2], 0.0)
        high = mix.astype(bf16)
        rest = (mix - high.astype(f32)).astype(bf16)

        def combine(step, carry, group=group, high=high, rest=rest, last=turn == visit_order[-1]):
            columns = pl.ds(pl.multiple_of(step * chunk, chunk), chunk)
            value = returned[group, :, columns]
            value = (
                total[:, columns]
                + jnp.dot(high, value, preferred_element_type=f32)
                + jnp.dot(rest, value, preferred_element_type=f32)
            )
            if last:
                result_ref[:, columns] = value.astype(bf16)
            else:
                total[:, columns] = value
            return carry

        lax.fori_loop(0, width // chunk, combine, 0)

    for turn in visit_order:
        count = size - 1 if turn == 0 else size
        finish(send_sem, 0, sent, sent_x, (my_group + turn) % groups, count)
        finish(send_sem, 1, answer, answer_x, (my_group + groups - turn) % groups, count)


def body(
    pool_input,
    stream_in,
    group_weight,
    pool_scale,
    out_weight,
    norm_gain,
    routes,
    route_weights,
    expert_gate,
    expert_up,
    expert_down,
):
    rows, pool_width = pool_input.shape
    width = stream_in.shape[1]
    ff = expert_gate.shape[2]
    n = lax.axis_size(("sp", "tp"))
    tp_size = lax.axis_size("tp")
    capacity = max(2, 3 * rows // n)
    main = capacity // 16 * 16
    extra = capacity - main
    size = n // groups
    per_group = size * capacity

    assigned = routes.T.reshape(-1)
    count = assigned.shape[0]
    order = jnp.arange(count, dtype=jnp.int32)
    same = (assigned[:, None] == assigned[None, :]) & (order[:, None] > order[None, :])
    earlier = jnp.sum(same.astype(jnp.int32), axis=1)
    place = assigned % size
    slot = (assigned // size) * per_group + jnp.where(
        earlier < main,
        place * main + earlier,
        size * main + place * extra + earlier - main,
    )
    slot_rows = slot.reshape(2, rows)

    bf16, f32 = jnp.bfloat16, jnp.float32
    vmem = pl.BlockSpec(memory_space=pltpu.VMEM)
    anywhere = pl.BlockSpec(memory_space=pl.ANY)
    slots = pltpu.VMEM((groups, per_group, width), bf16)
    slots_x = pltpu.VMEM((n, max(extra, 1), width), bf16)
    return pl.pallas_call(
        functools.partial(kernel, n, tp_size, main, extra),
        out_shape=jax.ShapeDtypeStruct((rows, width), bf16),
        in_specs=[
            anywhere,
            anywhere,
            anywhere,
            vmem,
            anywhere,
            vmem,
            vmem,
            vmem,
            vmem,
            anywhere,
            anywhere,
            anywhere,
        ],
        out_specs=vmem,
        scratch_shapes=[
            pltpu.VMEM((rows, pool_width), bf16),
            pltpu.VMEM((halo_rows, pool_width), bf16),
            pltpu.VMEM((halo_rows + rows, pool_width), f32),
            pltpu.VMEM((rows, width), bf16),
            pltpu.VMEM(group_weight.shape, bf16),
            pltpu.VMEM(out_weight.shape, bf16),
            pltpu.VMEM(expert_gate.shape[1:], bf16),
            pltpu.VMEM(expert_up.shape[1:], bf16),
            pltpu.VMEM(expert_down.shape[1:], bf16),
            pltpu.VMEM((rows, width), bf16),
            pltpu.VMEM((rows, pool_width), bf16),
            pltpu.VMEM((rows, width), f32),
            pltpu.VMEM((per_group, ff), bf16),
            slots,
            slots,
            slots,
            slots,
            slots_x,
            slots_x,
            slots_x,
            slots_x,
            pltpu.SemaphoreType.DMA((7,)),
            pltpu.SemaphoreType.DMA,
            pltpu.SemaphoreType.DMA,
            pltpu.SemaphoreType.DMA((2, 2)),
            pltpu.SemaphoreType.DMA((2, 2, groups)),
            pltpu.SemaphoreType.DMA((2, 2, groups)),
        ],
        compiler_params=pltpu.CompilerParams(
            collective_id=0, has_side_effects=True, vmem_limit_bytes=60 * 1024 * 1024
        ),
    )(
        pool_input,
        stream_in,
        group_weight,
        pool_scale[None, :],
        out_weight,
        norm_gain[None, :],
        slot_rows,
        slot_rows.T,
        route_weights,
        expert_gate,
        expert_up,
        expert_down,
    )


def solution(mesh):
    placed = (
        P(("sp", "tp"), None),
        P(("sp", "tp"), None),
        P(),
        P(),
        P(),
        P(),
        P(("sp", "tp"), None),
        P(("sp", "tp"), None),
        P(("sp", "tp"), None, None),
        P(("sp", "tp"), None, None),
        P(("sp", "tp"), None, None),
    )
    return jax.shard_map(
        body, mesh=mesh, in_specs=placed, out_specs=P(("sp", "tp"), None), check_vma=False
    )
```

```python
import functools

import jax
import jax.numpy as jnp
from jax import lax
from jax.experimental import pallas as pl
from jax.experimental.pallas import tpu as pltpu
from jax.sharding import PartitionSpec as P

MESH = pl.DeviceIdType.MESH
pool_windows = (2, 4, 8, 16)
halo_rows = 16
norm_epsilon = 1e-05
halves = 2
parts = 4
chunk = 256


def kernel(
    n,
    tp_size,
    main,
    extra,
    pool_hbm,
    stream_hbm,
    group_hbm,
    scale_ref,
    out_hbm,
    gain_ref,
    table_ref,
    gate_hbm,
    up_hbm,
    down_hbm,
    result_ref,
    pool_buf,
    halo_buf,
    extended,
    stream_buf,
    group_buf,
    outw_buf,
    gate_buf,
    up_buf,
    down_buf,
    normed_buf,
    grouped_buf,
    total,
    hidden_buf,
    sent,
    arrived,
    answer,
    returned,
    sent_x,
    arrived_x,
    answer_x,
    returned_x,
    raw_buf,
    mixed_buf,
    came_buf,
    far_table,
    load_sem,
    table_send,
    table_recv,
    mirror_send,
    mirror_recv,
    halo_send,
    halo_recv,
    own_sem,
    send_sem,
    recv_sem,
):
    f32, bf16 = jnp.float32, jnp.bfloat16
    rows, width = result_ref.shape
    pool_width = pool_buf.shape[1]
    group_width = pool_width // 4
    ff = hidden_buf.shape[1]
    size = n // halves
    per_half = size * (main + extra)
    edge = size * main

    me = lax.axis_index("sp") * tp_size + lax.axis_index("tp")
    my_half = me // size
    my_place = me % size

    def coordinates(device):
        return (device // tp_size, device % tp_size)

    mirror = coordinates((me + size) % n)

    loads = []
    for number, (source, target) in enumerate(
        (
            (pool_hbm, pool_buf),
            (group_hbm, group_buf),
            (out_hbm, outw_buf),
            (stream_hbm, stream_buf),
            (gate_hbm.at[0], gate_buf),
            (up_hbm.at[0], up_buf),
            (down_hbm.at[0], down_buf),
        )
    ):
        copy = pltpu.make_async_copy(source, target, load_sem.at[number])
        copy.start()
        loads.append(copy)

    barrier = pltpu.get_barrier_semaphore()

    def greet(step, carry):
        pl.semaphore_signal(
            barrier, inc=1, device_id=coordinates((me + step) % n), device_id_type=MESH
        )
        return carry

    lax.fori_loop(1, n, greet, 0)
    pl.semaphore_wait(barrier, n - 1)

    halo = pltpu.make_async_remote_copy(
        src_ref=pool_hbm.at[pl.ds(rows - halo_rows, halo_rows)],
        dst_ref=halo_buf,
        send_sem=halo_send,
        recv_sem=halo_recv,
        device_id=coordinates((me + 1) % n),
        device_id_type=MESH,
    )
    halo.start()
    table_copy = pltpu.make_async_remote_copy(
        src_ref=table_ref,
        dst_ref=far_table,
        send_sem=table_send,
        recv_sem=table_recv,
        device_id=mirror,
        device_id_type=MESH,
    )
    table_copy.start()

    loads[0].wait()
    extended[pl.ds(halo_rows, rows), :] = pool_buf[...].astype(f32)
    loads[1].wait()
    halo.wait()
    extended[pl.ds(0, halo_rows), :] = jnp.where(me > 0, halo_buf[...].astype(f32), 0.0)
    position = (me * rows + lax.broadcasted_iota(jnp.int32, (rows, 1), 0)).astype(f32)
    for index, window in enumerate(pool_windows):
        low = index * group_width
        columns = slice(low, low + group_width)
        own = extended[pl.ds(halo_rows, rows), columns]
        trail = own
        for lag in range(1, window):
            trail = trail + extended[pl.ds(halo_rows - lag, rows), columns]
        count = jnp.minimum(position + 1.0, float(window))
        pooled = (trail / count - own).astype(bf16)
        mapped = jnp.dot(pooled, group_buf[index], preferred_element_type=f32)
        grouped_buf[:, columns] = (mapped * scale_ref[:, columns]).astype(bf16)

    loads[2].wait()
    loads[3].wait()

    def project(step, square):
        columns = pl.ds(pl.multiple_of(step * chunk, chunk), chunk)
        value = stream_buf[:, columns].astype(f32) + jnp.dot(
            grouped_buf[...], outw_buf[:, columns], preferred_element_type=f32
        )
        value = value.astype(bf16).astype(f32)
        total[:, columns] = value
        return square + jnp.sum(value * value, axis=1, keepdims=True)

    square = lax.fori_loop(0, width // chunk, project, jnp.zeros((rows, 1), f32))
    scale = lax.rsqrt(square / width + norm_epsilon)
    normed_buf[...] = (total[...] * scale * gain_ref[...]).astype(bf16)

    def block(buffer, part, place, columns):
        return buffer.at[part, pl.ds(pl.multiple_of(place * main, 16), main), columns]

    def spread(buffer, buffer_x, part, columns):
        if extra:
            for place in range(size):
                start = edge + place * extra
                buffer_x[part, place, :, columns] = buffer[part, start : start + extra, columns]

    def gather(buffer, buffer_x, part, columns):
        if extra:
            for place in range(size):
                start = edge + place * extra
                buffer[part, start : start + extra, columns] = buffer_x[part, place, :, columns]

    def own_copies(way, source, source_x, target, target_x, part, columns, number):
        copies = []
        if main:
            copies.append(
                pltpu.make_async_copy(
                    block(source, part, my_place, columns),
                    block(target, part, my_place, columns),
                    own_sem.at[way, 0, number],
                )
            )
        if extra:
            copies.append(
                pltpu.make_async_copy(
                    source_x.at[part, my_place, :, columns],
                    target_x.at[part, my_place, :, columns],
                    own_sem.at[way, 1, number],
                )
            )
        return copies

    def exchange(way, source, source_x, target, target_x, part, columns, number):
        spread(source, source_x, part, columns)

        def one(step, carry):
            place = (my_place + step) % size
            peer = coordinates(my_half * size + place)
            if main:
                pltpu.make_async_remote_copy(
                    src_ref=block(source, part, place, columns),
                    dst_ref=block(target, part, my_place, columns),
                    send_sem=send_sem.at[way, 0, number],
                    recv_sem=recv_sem.at[way, 0, number],
                    device_id=peer,
                    device_id_type=MESH,
                ).start()
            if extra:
                pltpu.make_async_remote_copy(
                    src_ref=source_x.at[part, place, :, columns],
                    dst_ref=target_x.at[part, my_place, :, columns],
                    send_sem=send_sem.at[way, 1, number],
                    recv_sem=recv_sem.at[way, 1, number],
                    device_id=peer,
                    device_id_type=MESH,
                ).start()
            return carry

        lax.fori_loop(1, size, one, 0)
        for copy in own_copies(way, source, source_x, target, target_x, part, columns, number):
            copy.start()

    def finish(semaphore, way, buffer, buffer_x, part, columns, number):
        if main:
            span = buffer.at[part, pl.ds(0, (size - 1) * main), columns]
            pltpu.make_async_copy(span, span, semaphore.at[way, 0, number]).wait()
        if extra:
            span = buffer_x.at[part, pl.ds(0, size - 1), :, columns]
            pltpu.make_async_copy(span, span, semaphore.at[way, 1, number]).wait()

    def receive(way, source, source_x, target, target_x, part, columns, number):
        finish(recv_sem, way, target, target_x, part, columns, number)
        for copy in own_copies(way, source, source_x, target, target_x, part, columns, number):
            copy.wait()
        gather(target, target_x, part, columns)

    def to_mirror(source, target, number, columns):
        return pltpu.make_async_remote_copy(
            src_ref=source.at[:, columns],
            dst_ref=target.at[:, columns],
            send_sem=mirror_send.at[number],
            recv_sem=mirror_recv.at[number],
            device_id=mirror,
            device_id_type=MESH,
        )

    whole = slice(0, width)
    part_width = width // parts
    pieces = [slice(c * part_width, (c + 1) * part_width) for c in range(parts)]
    out_raw = [to_mirror(normed_buf, raw_buf, c, pieces[c]) for c in range(parts)]
    out_sum = [to_mirror(mixed_buf, came_buf, parts + c, pieces[c]) for c in range(parts)]

    base = my_half * per_half
    wanted = (base + lax.broadcasted_iota(jnp.int32, (per_half, rows), 0)).astype(f32)

    def chosen(table):
        hit = (wanted == table[0:1, :]) | (wanted == table[1:2, :])
        return jnp.where(hit, 1.0, 0.0).astype(bf16)

    def mixing(table):
        mix = jnp.where(wanted == table[0:1, :], table[2:3, :], 0.0)
        mix = mix + jnp.where(wanted == table[1:2, :], table[3:4, :], 0.0)
        high = mix.astype(bf16)
        return high, (mix - high.astype(f32)).astype(bf16)

    def weigh(mix, value):
        dims = (((0,), (0,)), ((), ()))
        first = lax.dot_general(mix[0], value, dims, preferred_element_type=f32)
        return first + lax.dot_general(mix[1], value, dims, preferred_element_type=f32)

    def hide(part):
        def one(step, carry):
            columns = pl.ds(pl.multiple_of(step * chunk, chunk), chunk)
            inputs = arrived[part]
            gate = jnp.dot(inputs, gate_buf[:, columns], preferred_element_type=f32)
            upward = jnp.dot(inputs, up_buf[:, columns], preferred_element_type=f32)
            hidden_buf[:, columns] = (gate / (1.0 + jnp.exp(-gate)) * upward).astype(bf16)
            return carry

        lax.fori_loop(0, ff // chunk, one, 0)

    there = (sent, sent_x, arrived, arrived_x)
    back = (answer, answer_x, returned, returned_x)

    own_chosen = chosen(table_ref)
    for columns in pieces:
        sent[0, :, columns] = jnp.dot(
            own_chosen, normed_buf[:, columns], preferred_element_type=f32
        ).astype(bf16)
    exchange(0, *there, 0, whole, 0)
    for copy in out_raw:
        copy.start()

    table_copy.wait()
    far_chosen = chosen(far_table)

    def serve_own():
        for copy in loads[4:]:
            copy.wait()
        receive(0, *there, 0, whole, 0)
        hide(0)
        for columns in pieces:
            answer[0, :, columns] = jnp.dot(
                hidden_buf[...], down_buf[:, columns], preferred_element_type=f32
            ).astype(bf16)
        exchange(1, *back, 0, whole, 0)

    for c, columns in enumerate(pieces):
        out_raw[c].wait_recv()
        sent[1, :, columns] = jnp.dot(
            far_chosen, raw_buf[:, columns], preferred_element_type=f32
        ).astype(bf16)
        exchange(0, *there, 1, columns, 1 + c)
        if c == parts - 1:
            serve_own()

    for c, columns in enumerate(pieces):
        receive(0, *there, 1, columns, 1 + c)
    hide(1)
    for c, columns in enumerate(pieces):
        answer[1, :, columns] = jnp.dot(
            hidden_buf[...], down_buf[:, columns], preferred_element_type=f32
        ).astype(bf16)
        exchange(1, *back, 1, columns, 1 + c)

    far_mix = mixing(far_table)
    for c, columns in enumerate(pieces):
        receive(1, *back, 1, columns, 1 + c)
        mixed_buf[:, columns] = weigh(far_mix, returned[1, :, columns]).astype(bf16)
        out_sum[c].start()

    receive(1, *back, 0, whole, 0)
    own_mix = mixing(table_ref)
    for columns in pieces:
        total[:, columns] = total[:, columns] + weigh(own_mix, returned[0, :, columns])

    for c, columns in enumerate(pieces):
        out_sum[c].wait_recv()
        result_ref[:, columns] = (total[:, columns] + came_buf[:, columns].astype(f32)).astype(bf16)

    for c in range(parts):
        out_raw[c].wait_send()
        out_sum[c].wait_send()
    for way, source, source_x in ((0, sent, sent_x), (1, answer, answer_x)):
        finish(send_sem, way, source, source_x, 0, whole, 0)
        for c, columns in enumerate(pieces):
            finish(send_sem, way, source, source_x, 1, columns, 1 + c)


def body(
    pool_input,
    stream_in,
    group_weight,
    pool_scale,
    out_weight,
    norm_gain,
    routes,
    route_weights,
    expert_gate,
    expert_up,
    expert_down,
):
    rows, pool_width = pool_input.shape
    width = stream_in.shape[1]
    ff = expert_gate.shape[2]
    n = lax.axis_size(("sp", "tp"))
    tp_size = lax.axis_size("tp")
    capacity = max(2, 3 * rows // n)
    main = capacity // 16 * 16
    extra = capacity - main
    size = n // halves
    per_half = size * capacity

    assigned = routes.T.reshape(-1)
    count = assigned.shape[0]
    order = jnp.arange(count, dtype=jnp.int32)
    same = (assigned[:, None] == assigned[None, :]) & (order[:, None] > order[None, :])
    earlier = jnp.sum(same.astype(jnp.int32), axis=1)
    place = assigned % size
    slot = (assigned // size) * per_half + jnp.where(
        earlier < main,
        place * main + earlier,
        size * main + place * extra + earlier - main,
    )
    table = jnp.concatenate(
        [
            slot.reshape(2, rows).astype(jnp.float32),
            route_weights.T,
            jnp.zeros((4, rows), jnp.float32),
        ]
    )

    bf16, f32 = jnp.bfloat16, jnp.float32
    vmem = pl.BlockSpec(memory_space=pltpu.VMEM)
    anywhere = pl.BlockSpec(memory_space=pl.ANY)
    slots = pltpu.VMEM((halves, per_half, width), bf16)
    slots_x = pltpu.VMEM((halves, size, max(extra, 1), width), bf16)
    return pl.pallas_call(
        functools.partial(kernel, n, tp_size, main, extra),
        out_shape=jax.ShapeDtypeStruct((rows, width), bf16),
        in_specs=[
            anywhere,
            anywhere,
            anywhere,
            vmem,
            anywhere,
            vmem,
            vmem,
            anywhere,
            anywhere,
            anywhere,
        ],
        out_specs=vmem,
        scratch_shapes=[
            pltpu.VMEM((rows, pool_width), bf16),
            pltpu.VMEM((halo_rows, pool_width), bf16),
            pltpu.VMEM((halo_rows + rows, pool_width), f32),
            pltpu.VMEM((rows, width), bf16),
            pltpu.VMEM(group_weight.shape, bf16),
            pltpu.VMEM(out_weight.shape, bf16),
            pltpu.VMEM(expert_gate.shape[1:], bf16),
            pltpu.VMEM(expert_up.shape[1:], bf16),
            pltpu.VMEM(expert_down.shape[1:], bf16),
            pltpu.VMEM((rows, width), bf16),
            pltpu.VMEM((rows, pool_width), bf16),
            pltpu.VMEM((rows, width), f32),
            pltpu.VMEM((per_half, ff), bf16),
            slots,
            slots,
            slots,
            slots,
            slots_x,
            slots_x,
            slots_x,
            slots_x,
            pltpu.VMEM((rows, width), bf16),
            pltpu.VMEM((rows, width), bf16),
            pltpu.VMEM((rows, width), bf16),
            pltpu.VMEM((8, rows), f32),
            pltpu.SemaphoreType.DMA((7,)),
            pltpu.SemaphoreType.DMA,
            pltpu.SemaphoreType.DMA,
            pltpu.SemaphoreType.DMA((2 * parts,)),
            pltpu.SemaphoreType.DMA((2 * parts,)),
            pltpu.SemaphoreType.DMA,
            pltpu.SemaphoreType.DMA,
            pltpu.SemaphoreType.DMA((2, 2, 1 + parts)),
            pltpu.SemaphoreType.DMA((2, 2, 1 + parts)),
            pltpu.SemaphoreType.DMA((2, 2, 1 + parts)),
        ],
        compiler_params=pltpu.CompilerParams(
            collective_id=0, has_side_effects=True, vmem_limit_bytes=60 * 1024 * 1024
        ),
    )(
        pool_input,
        stream_in,
        group_weight,
        pool_scale[None, :],
        out_weight,
        norm_gain[None, :],
        table,
        expert_gate,
        expert_up,
        expert_down,
    )


def solution(mesh):
    placed = (
        P(("sp", "tp"), None),
        P(("sp", "tp"), None),
        P(),
        P(),
        P(),
        P(),
        P(("sp", "tp"), None),
        P(("sp", "tp"), None),
        P(("sp", "tp"), None, None),
        P(("sp", "tp"), None, None),
        P(("sp", "tp"), None, None),
    )
    return jax.shard_map(
        body, mesh=mesh, in_specs=placed, out_specs=P(("sp", "tp"), None), check_vma=False
    )
```
